32 devices in a mesh: sp: 16 (over z, y, x), tp: 2 (over core).
Axes of the slice: x: 2, y: 2, z: 4, core: 2. Of those that a mesh axis runs over, the one named last changes fastest.
Arguments:
- query_heads: bfloat16 [2048, 1024], P('sp', 'tp'), may hold values from -12 to 12
- key_heads: bfloat16 [2048, 1024], P('sp', 'tp'), may hold values from -6 to 6
- value_heads: bfloat16 [2048, 1024], P('sp', 'tp'), may hold values from -6 to 6
- decay_sums: float32 [2048, 8], P('sp', 'tp'), may hold values from -338 to 0, as said below
- row_logsums: float32 [2048, 8], P('sp', 'tp'), may hold values from -9216 to 11264, as said below
- head_outputs: bfloat16 [2048, 1024], P('sp', 'tp'), may hold values from -1.796875 to 1.796875
- out_cotangent: bfloat16 [2048, 1024], P('sp', 'tp'), may hold values from -24 to 24
- normed_input: bfloat16 [2048, 2048], P('sp', 'tp'), may hold values from -6 to 6
Outputs:
- query_grads: bfloat16 [2048, 1024], P('sp', 'tp')
- key_grads: bfloat16 [2048, 1024], P('sp', 'tp')
- value_grads: bfloat16 [2048, 1024], P('sp', 'tp')
- weight_grad: float32 [2048, 1024], P('sp', 'tp')
The draws below stay inside these ranges and needn't reach their ends.
Inputs may be any that keep to these rules, and one draw needn't show every extreme that they name: `decay_sums`: each head's values never rise along the positions. `row_logsums`: each entry is the logarithm of the sum, over key positions up to the row's own, of the exponentials of score_scale times the inner product plus the gate difference, as in the reference program.
All inputs are finite; a program needn't handle non-finite values.
Results may differ from the reference program's by a relative error of at most 0.005.
Values may be sent and summed in bfloat16 or wider, within the bound.
A program may use at most 64 MiB of HBM per device.

```python
import jax
import jax.numpy as jnp
from jax import lax

D = 2048
HEAD_TOTAL = 8
HEAD_SIZE = 128
TOK_DEV = 128
TOKEN_TOTAL = 2048


def head_inputs(key):
    queries = jax.random.normal(jax.random.fold_in(key, 11), (TOKEN_TOTAL, HEAD_TOTAL * HEAD_SIZE), jnp.float32)
    keys_drawn = jax.random.normal(jax.random.fold_in(key, 12), (TOKEN_TOTAL, HEAD_TOTAL * HEAD_SIZE), jnp.float32)
    queries = jnp.clip(queries, -6.0, 6.0)
    keys_drawn = jnp.clip(keys_drawn, -6.0, 6.0)
    return (queries.astype(jnp.bfloat16), keys_drawn.astype(jnp.bfloat16))


def gate_totals(key):
    order = jax.random.permutation(jax.random.fold_in(key, 21), HEAD_TOTAL)
    fast_count = HEAD_TOTAL // 2
    fast = order < fast_count
    slow_rate = jnp.exp(jax.random.uniform(jax.random.fold_in(key, 22), (HEAD_TOTAL,), jnp.float32, -1.204, -0.223)) / TOKEN_TOTAL
    fast_rate = jnp.exp(jax.random.uniform(jax.random.fold_in(key, 23), (HEAD_TOTAL,), jnp.float32, 0.693, 1.792)) / TOK_DEV
    rate = jnp.where(fast, fast_rate, slow_rate)
    block_factor = jnp.exp(jax.random.uniform(jax.random.fold_in(key, 24), (TOKEN_TOTAL // TOK_DEV, 1, HEAD_TOTAL), jnp.float32, -0.693, 0.693))
    position_factor = jax.random.uniform(jax.random.fold_in(key, 25), (TOKEN_TOTAL // TOK_DEV, TOK_DEV, HEAD_TOTAL), jnp.float32, 0.3, 1.7)
    step_amount = (rate * block_factor * position_factor).reshape(TOKEN_TOTAL, HEAD_TOTAL)
    spike_location = jax.random.randint(jax.random.fold_in(key, 26), (2, 1, HEAD_TOTAL), 0, TOKEN_TOTAL)
    spike_penalty = -jnp.log(1.0 - jax.random.uniform(jax.random.fold_in(key, 27), (2, 1, HEAD_TOTAL), jnp.float32, 0.2, 0.4))
    token_places = jnp.arange(TOKEN_TOTAL, dtype=jnp.int32)[None, :, None]
    spike_events = jnp.sum(jnp.where(token_places == spike_location, spike_penalty, 0.0), axis=0)
    return jnp.cumsum(-(step_amount + spike_events), axis=0)


def draw_query_heads(key, part):
    return head_inputs(key)[0]


def draw_key_heads(key, part):
    return head_inputs(key)[1]


def draw_decay_sums(key, part):
    return gate_totals(key)


def draw_row_logsums(key, part):
    queries, keys_drawn = head_inputs(key)
    gates = gate_totals(key)
    query_rows = queries.astype(jnp.float32).reshape(TOKEN_TOTAL, HEAD_TOTAL, HEAD_SIZE)
    key_rows = keys_drawn.astype(jnp.float32).reshape(TOKEN_TOTAL, HEAD_TOTAL, HEAD_SIZE)
    length = TOKEN_TOTAL
    while length > 256 and length % 2 == 0:
        length = length // 2
    token_places = jnp.arange(TOKEN_TOTAL, dtype=jnp.int32)

    def one_block(first_row):
        query_part = lax.dynamic_slice_in_dim(query_rows, first_row, length, 0)
        gate_part = lax.dynamic_slice_in_dim(gates, first_row, length, 0)
        scores = jnp.einsum('ahd,bhd->hab', query_part, key_rows) * HEAD_SIZE ** (-0.5)
        scores = scores + (gate_part.T[:, :, None] - gates.T[:, None, :])
        query_pos = first_row + jnp.arange(length, dtype=jnp.int32)
        allowed = token_places[None, None, :] <= query_pos[None, :, None]
        scores = jnp.where(allowed, scores, -jnp.inf)
        return jax.nn.logsumexp(scores, axis=2).T
    blocks = lax.map(one_block, jnp.arange(TOKEN_TOTAL // length, dtype=jnp.int32) * length)
    return blocks.reshape(TOKEN_TOTAL, HEAD_TOTAL)


def raised(values, stream_key, source, target, blocks, factor):
    def block_of(dim):
        return (jnp.arange(values.shape[dim]) // (values.shape[dim] // blocks)).reshape((-1,) + (1,) * (values.ndim - 1 - dim))

    near = jax.random.permutation(stream_key, blocks)[block_of(target)]
    second = (block_of(target) + blocks // 2) % blocks
    return jnp.where((block_of(source) == near) | (block_of(source) == second), factor * values, values)


def block_levels(own_key, extent, cuts, smallest, top_value):
    def one(position, parts):
        heights = jax.random.uniform(jax.random.fold_in(jax.random.fold_in(own_key, 6), position), (parts,), jnp.float32, smallest / len(cuts), top_value / len(cuts))
        return jnp.repeat(jnp.exp(heights), extent[position] // parts).reshape((-1,) + (1,) * (len(extent) - position - 1))

    gain = one(*cuts[0])
    for cut in cuts[1:]:
        gain = gain * one(*cut)
    return gain


def centred(stream_key, shape, spread, limit, pieces=(), held_as=jnp.bfloat16):
    result = spread * jax.random.normal(stream_key, shape, jnp.float32)
    if pieces:
        result = result * block_levels(stream_key, shape, pieces, -0.22, 0.18)
    return jnp.clip(result, -limit, limit).astype(held_as)


def heavy_noise(rng, extent, scale, bound, cuts, heavy, kind=jnp.bfloat16):
    values = scale * jax.random.normal(rng, extent, jnp.float32)
    if cuts:
        values = values * block_levels(rng, extent, cuts, -0.22, 0.18)
    return jnp.clip(raised(values, jax.random.fold_in(rng, 3), *heavy), -bound, bound).astype(kind)


def setup_inputs(seed: int = 0) -> dict:
    seeds = jax.random.split(jax.random.key(seed), 9)
    query_heads = draw_query_heads(jax.random.fold_in(seeds[8], 71), 0)
    key_heads = draw_key_heads(jax.random.fold_in(seeds[8], 71), 0)
    value_heads = centred(seeds[2], (TOKEN_TOTAL, HEAD_TOTAL * HEAD_SIZE), 1.0, 6.0, ((0, 16), (1, 2)))
    decay_sums = draw_decay_sums(jax.random.fold_in(seeds[8], 71), 0)
    row_logsums = draw_row_logsums(jax.random.fold_in(seeds[8], 71), 0)
    head_outputs = centred(seeds[5], (TOKEN_TOTAL, HEAD_TOTAL * HEAD_SIZE), 0.3, 1.796875, ((0, 16), (1, 2)))
    out_cotangent = heavy_noise(seeds[6], (TOKEN_TOTAL, HEAD_TOTAL * HEAD_SIZE), 4.0, 24.0, ((0, 16), (1, 2)), (0, 1, 16, 2.0))
    normed_input = heavy_noise(seeds[7], (TOKEN_TOTAL, D), 1.0, 6.0, ((0, 16), (1, 2)), (0, 1, 16, 2.0))
    return {"query_heads": query_heads, "key_heads": key_heads, "value_heads": value_heads, "decay_sums": decay_sums, "row_logsums": row_logsums, "head_outputs": head_outputs, "out_cotangent": out_cotangent, "normed_input": normed_input}


def rounded(values):
    return lax.optimization_barrier(values.astype(jnp.bfloat16)).astype(jnp.float32)


def reference(query_heads, key_heads, value_heads, decay_sums, row_logsums, head_outputs, out_cotangent, normed_input):
    token_count, row_width = query_heads.shape
    head_count = decay_sums.shape[1]
    head_width = row_width // head_count
    score_scale = head_width ** -0.5
    shape = (token_count, head_count, head_width)
    queries_all = query_heads.astype(jnp.float32).reshape(shape)
    keys_all = key_heads.astype(jnp.float32).reshape(shape)
    values_all = value_heads.astype(jnp.float32).reshape(shape)
    grads_all = out_cotangent.astype(jnp.float32).reshape(shape)
    outputs_all = head_outputs.astype(jnp.float32).reshape(shape)
    row_terms = jnp.sum(outputs_all * grads_all, axis=2)
    token_places = jnp.arange(token_count, dtype=jnp.int32)
    length = token_count
    while length > 256 and length % 2 == 0:
        length = length // 2
    number = token_count // length

    def visit_one(running, first_row):
        key_sum, value_sum = running
        query_part = lax.dynamic_slice_in_dim(queries_all, first_row, length, 0)
        grad_part = lax.dynamic_slice_in_dim(grads_all, first_row, length, 0)
        gate_part = lax.dynamic_slice_in_dim(decay_sums, first_row, length, 0)
        norm_part = lax.dynamic_slice_in_dim(row_logsums, first_row, length, 0)
        term_part = lax.dynamic_slice_in_dim(row_terms, first_row, length, 0)
        query_pos = first_row + jnp.arange(length, dtype=jnp.int32)
        scores = jnp.einsum("ahd,bhd->hab", query_part, keys_all) * score_scale
        scores = scores + (gate_part.T[:, :, None] - decay_sums.T[:, None, :])
        allowed = token_places[None, None, :] <= query_pos[None, :, None]
        weights = jnp.exp(jnp.where(allowed, scores - norm_part.T[:, :, None], -jnp.inf))
        flows = jnp.einsum("ahd,bhd->hab", grad_part, values_all)
        slopes = weights * (flows - term_part.T[:, :, None])
        slopes_low = rounded(slopes)
        weights_low = rounded(weights)
        query_block = (jnp.einsum("hab,bhd->ahd", slopes_low, keys_all) * score_scale).astype(jnp.bfloat16)
        key_sum = key_sum + jnp.einsum("hab,ahd->bhd", slopes_low, query_part)
        value_sum = value_sum + jnp.einsum("hab,ahd->bhd", weights_low, grad_part)
        return (key_sum, value_sum), query_block

    zero_sums = jnp.zeros(shape, jnp.float32)
    starts = jnp.arange(number, dtype=jnp.int32) * length
    (key_sum, value_sum), query_blocks = lax.scan(visit_one, (zero_sums, zero_sums), starts)
    query_grads = query_blocks.reshape(token_count, row_width)
    key_grads = (key_sum * score_scale).astype(jnp.bfloat16).reshape(token_count, row_width)
    value_grads = value_sum.astype(jnp.bfloat16).reshape(token_count, row_width)
    weight_grad = jnp.dot(normed_input.T, query_grads, preferred_element_type=jnp.float32)
    return query_grads, key_grads, value_grads, weight_grad
```

```python
import functools

import jax
import jax.numpy as jnp
from jax import lax
from jax.experimental import pallas as pl
from jax.experimental.pallas import tpu as pltpu
from jax.sharding import PartitionSpec as P


def block_length(whole_rows):
    length = whole_rows
    while length > 1024 and length % 2 == 0:
        length = length // 2
    return length


def split_heads(block, head_count):
    return block.reshape(block.shape[0], head_count, block.shape[1] // head_count)


def attention_weights(
    query_part, key_part, norm_part, gate_query, gate_key, query_pos, key_pos, score_scale
):
    scores = (
        jnp.einsum("ahd,bhd->hab", query_part, key_part, preferred_element_type=jnp.float32)
        * score_scale
    )
    scores = scores + (gate_query.T[:, :, None] - gate_key.T[:, None, :])
    allowed = key_pos[None, None, :] <= query_pos[None, :, None]
    return jnp.exp(jnp.where(allowed, scores - norm_part.T[:, :, None], -jnp.inf))


def score_slopes(weights, grad_part, value_part, term_part):
    flows = jnp.einsum("ahd,bhd->hab", grad_part, value_part, preferred_element_type=jnp.float32)
    return weights * (flows - term_part.T[:, :, None])


def over_blocks(visit_block, running, members):
    whole_rows = members[0].shape[0]
    length = block_length(whole_rows)
    number = whole_rows // length
    stacked = tuple((member.reshape((number, length) + member.shape[1:]) for member in members))

    def visit_one(carried, scanned):
        block_index, block_parts = scanned
        token_places = block_index * length + jnp.arange(length, dtype=jnp.int32)
        return (visit_block(carried, block_parts, token_places), None)

    result, unused = lax.scan(visit_one, running, (jnp.arange(number, dtype=jnp.int32), stacked))
    return result


def gathered_device(
    query_heads,
    key_heads,
    value_heads,
    decay_sums,
    row_logsums,
    head_outputs,
    out_cotangent,
    normed_input,
):
    own_rows, row_width = query_heads.shape
    head_count = decay_sums.shape[1]
    score_scale = (row_width // head_count) ** (-0.5)
    own_pos = lax.axis_index("sp") * own_rows + jnp.arange(own_rows, dtype=jnp.int32)
    own_query = split_heads(query_heads, head_count)
    own_key = split_heads(key_heads, head_count)
    own_value = split_heads(value_heads, head_count)
    own_grad = split_heads(out_cotangent, head_count)
    row_terms = jnp.einsum(
        "ahd,ahd->ah",
        split_heads(head_outputs, head_count),
        own_grad,
        preferred_element_type=jnp.float32,
    )
    all_gates, all_logsums, all_terms = (
        lax.all_gather(decay_sums, "sp", axis=0, tiled=True),
        lax.all_gather(row_logsums, "sp", axis=0, tiled=True),
        lax.all_gather(row_terms, "sp", axis=0, tiled=True),
    )

    def query_side(query_sum, key_part, value_part, key_pos):
        gate_key = lax.dynamic_slice_in_dim(all_gates, key_pos[0], key_pos.shape[0], 0)

        def query_compute(running):
            weights = attention_weights(
                own_query,
                key_part,
                row_logsums,
                decay_sums,
                gate_key,
                own_pos,
                key_pos,
                score_scale,
            )
            slopes = score_slopes(weights, own_grad, value_part, row_terms)
            return running + jnp.einsum(
                "hab,bhd->ahd",
                slopes.astype(jnp.bfloat16),
                key_part,
                preferred_element_type=jnp.float32,
            )

        return lax.cond(
            key_pos[0] <= own_pos[-1], query_compute, lambda running: running, query_sum
        )

    def key_side(key_sums, query_part, grad_part, query_pos):
        length = query_pos.shape[0]
        gate_query = lax.dynamic_slice_in_dim(all_gates, query_pos[0], length, 0)
        norm_part = lax.dynamic_slice_in_dim(all_logsums, query_pos[0], length, 0)
        term_part = lax.dynamic_slice_in_dim(all_terms, query_pos[0], length, 0)

        def key_compute(running):
            key_sum, value_sum = running
            weights = attention_weights(
                query_part,
                own_key,
                norm_part,
                gate_query,
                decay_sums,
                query_pos,
                own_pos,
                score_scale,
            )
            slopes = score_slopes(weights, grad_part, own_value, term_part)
            key_sum = key_sum + jnp.einsum(
                "hab,ahd->bhd",
                slopes.astype(jnp.bfloat16),
                query_part,
                preferred_element_type=jnp.float32,
            )
            value_sum = value_sum + jnp.einsum(
                "hab,ahd->bhd",
                weights.astype(jnp.bfloat16),
                grad_part,
                preferred_element_type=jnp.float32,
            )
            return (key_sum, value_sum)

        return lax.cond(query_pos[-1] >= own_pos[0], key_compute, lambda running: running, key_sums)

    zero_sums = jnp.zeros((own_rows, head_count, row_width // head_count), jnp.float32)

    def visit_block(carried, block_parts, token_places):
        return query_side(
            carried,
            split_heads(block_parts[0], head_count),
            split_heads(block_parts[1], head_count),
            token_places,
        )

    query_sum = over_blocks(
        visit_block,
        zero_sums,
        (
            lax.all_gather(key_heads, "sp", axis=0, tiled=True),
            lax.all_gather(value_heads, "sp", axis=0, tiled=True),
        ),
    )

    def visit_block(carried, block_parts, token_places):
        return key_side(
            carried,
            split_heads(block_parts[0], head_count),
            split_heads(block_parts[1], head_count),
            token_places,
        )

    key_sum, value_sum = over_blocks(
        visit_block,
        (zero_sums, zero_sums),
        (
            lax.all_gather(query_heads, "sp", axis=0, tiled=True),
            lax.all_gather(out_cotangent, "sp", axis=0, tiled=True),
        ),
    )
    query_grads = (query_sum * score_scale).astype(jnp.bfloat16).reshape(own_rows, row_width)
    key_grads = (key_sum * score_scale).astype(jnp.bfloat16).reshape(own_rows, row_width)
    value_grads = value_sum.astype(jnp.bfloat16).reshape(own_rows, row_width)
    whole_input = lax.all_gather(normed_input, "tp", axis=1, tiled=True)
    own_features = lax.all_to_all(whole_input, "sp", split_axis=1, concat_axis=0, tiled=True)
    weight_grad = lax.dot_general(
        own_features,
        lax.all_gather(query_grads, "sp", axis=0, tiled=True),
        (((0,), (0,)), ((), ())),
        preferred_element_type=jnp.float32,
    )
    return (query_grads, key_grads, value_grads, weight_grad)


F32 = jnp.float32
BF16 = jnp.bfloat16


def dot_last(a, b):
    return lax.dot_general(a, b, (((1,), (1,)), ((), ())), preferred_element_type=F32)


def dot_plain(a, b):
    return lax.dot_general(a, b, (((1,), (0,)), ((), ())), preferred_element_type=F32)


def dot_first(a, b):
    return lax.dot_general(a, b, (((0,), (0,)), ((), ())), preferred_element_type=F32)


def fused_kernel(
    sp, tp, u, n, hd,
    q_ref, k_ref, v_ref, g_ref, l_ref, o_ref, do_ref, x_ref,
    dq_out, dk_out, dv_out, w_out,
    kbuf, vbuf, qbuf, dobuf, sbuf, ssend, tmp, cols, xbuf, dqpair, dkv, acc, wsend, wrecv,
    main_send, main_recv, stat_send, stat_recv, x_send, x_recv,
    pair_send, pair_recv, out_send, out_recv, w_send, w_recv,
):
    r = sp // u
    length = u * n
    owners = sp // tp
    fw = x_ref.shape[1] // owners
    scale = hd ** (-0.5)
    me, p = lax.axis_index("sp"), lax.axis_index("tp")
    z, g = me // u, me % u

    def lanes(index, width=hd):
        return pl.ds(pl.multiple_of(index * width, width), width)

    def rows(index):
        return pl.ds(pl.multiple_of(index * n, n), n)

    def remote(src, dst, send, recv, i, t):
        return pltpu.make_async_remote_copy(
            src_ref=src, dst_ref=dst, send_sem=send, recv_sem=recv,
            device_id={"sp": i, "tp": t}, device_id_type=pl.DeviceIdType.MESH,
        )

    barrier = pltpu.get_barrier_semaphore()
    for d in range(1, sp * tp):
        other = lax.rem(me * tp + p + d, sp * tp)
        pl.semaphore_signal(
            barrier, inc=1, device_id={"sp": other // tp, "tp": other % tp},
            device_id_type=pl.DeviceIdType.MESH,
        )

    lane = lax.broadcasted_iota(jnp.int32, (n, hd), 1)
    terms = jnp.zeros((n, hd), F32)
    for h in range(u):
        part = slice(h * hd, (h + 1) * hd)
        total = jnp.sum(
            o_ref[:, part].astype(F32) * do_ref[:, part].astype(F32), axis=1, keepdims=True
        )
        terms = jnp.where(lane == h, total, terms)
    tmp[0] = jnp.zeros((n, hd), F32)
    tmp[1] = jnp.zeros((n, hd), F32)
    tmp[0, :, 0:u] = g_ref[...]
    tmp[1, :, 0:u] = g_ref[...] - l_ref[...]
    flat = (tmp[0].T, tmp[1].T, terms.T)
    for h in range(u):
        for s in range(3):
            ssend[h, s : s + 1, :] = flat[s][h : h + 1, :]
    pl.semaphore_wait(barrier, sp * tp - 1)

    def head_of(j):
        return lax.rem(g + j, u)

    def source_of(j):
        return lax.rem(g + u - j, u)

    pairs = ((k_ref, kbuf), (v_ref, vbuf), (q_ref, qbuf), (do_ref, dobuf))

    def main_copy(a, k, j):
        ref, buf = pairs[a]
        layer = z + k if a < 2 else z - k
        h = head_of(j)
        return remote(
            ref.at[:, lanes(h)], buf.at[z, rows(g), :],
            main_send.at[a, k, j], main_recv.at[a, k, j], layer * u + h, p,
        )

    def own_copy(a):
        ref, buf = pairs[a]
        return pltpu.make_async_copy(
            ref.at[:, lanes(g)], buf.at[z, rows(g), :], main_recv.at[a, 0, 0]
        )

    def wait_main(a, k, j):
        ref, buf = pairs[a]
        layer = z - k if a < 2 else z + k
        here = buf.at[layer, rows(source_of(j)), :]
        pltpu.make_async_copy(here, here, main_recv.at[a, k, j]).wait()

    def stat_copy(d, j):
        h = head_of(j)
        return remote(
            ssend.at[h], sbuf.at[me], stat_send.at[d + r - 1, j], stat_recv.at[d + r - 1, j],
            (z + d) * u + h, p,
        )

    def wait_stat(d, j):
        here = sbuf.at[(z - d) * u + source_of(j)]
        pltpu.make_async_copy(here, here, stat_recv.at[d + r - 1, j]).wait()

    def own_stat():
        return pltpu.make_async_copy(ssend.at[g], sbuf.at[me], stat_recv.at[r - 1, 0])

    def x_copy(j):
        return remote(
            x_ref, xbuf.at[rows(g), :], x_send.at[j], x_recv.at[j], z * u + head_of(j), p
        )

    def up(k):
        return z + k < r

    def down(k):
        return z >= k

    def each_send(act):
        for j in range(1, u):
            act(stat_copy(0, j))
        for a in (2, 0, 3, 1):
            for j in range(1, u):
                act(main_copy(a, 0, j))
        for k in range(1, r):
            for reach, sign, members in ((up, 1, (0, 1)), (down, -1, (2, 3))):

                @pl.when(reach(k))
                def _(k=k, sign=sign, members=members):
                    for j in range(u):
                        act(stat_copy(sign * k, j))
                    for a in members:
                        for j in range(u):
                            act(main_copy(a, k, j))

        for j in range(1, u):
            act(x_copy(j))

    each_send(lambda copy: copy.start())
    own_stat().start()
    for a in range(4):
        own_copy(a).start()
    own_x = pltpu.make_async_copy(x_ref, xbuf.at[rows(g), :], x_recv.at[0])
    own_x.start()

    for j in range(u):
        wait_stat(0, j)
        for a in range(4):
            wait_main(a, 0, j)
    for b in range(u):
        for s in range(3):
            row = sbuf[z * u + b, s : s + 1, :]
            cols[s, b * n : (b + 1) * n, :] = jnp.broadcast_to(row, (hd, n)).T

    width = 2 * n if u % 2 == 0 else n
    pieces = width // n

    def stat_row(s, layer, c):
        return jnp.concatenate(
            [sbuf[layer * u + c * pieces + i, s : s + 1, :] for i in range(pieces)], axis=1
        )

    def wide(s, part):
        return jnp.concatenate([cols[s, part, :]] * pieces, axis=1)

    def query_tile(b, c, part, masked):
        keys = slice(c * width, (c + 1) * width)
        kk, vv = kbuf[b, keys, :], vbuf[b, keys, :]
        scores = dot_last(qbuf[z, part, :], kk) * scale + (wide(1, part) - stat_row(0, b, c))
        if masked:
            t = lax.broadcasted_iota(jnp.int32, scores.shape, 0) + part.start
            s = lax.broadcasted_iota(jnp.int32, scores.shape, 1) + c * width
            scores = jnp.where(s <= t, scores, -jnp.inf)
        slopes = jnp.exp(scores) * (dot_last(dobuf[z, part, :], vv) - wide(2, part))
        acc[0, part, :] += dot_plain(slopes.astype(BF16), kk)

    def key_tile(a, c, part, masked):
        span = slice(c * width, (c + 1) * width)
        qq, dd = qbuf[a, span, :], dobuf[a, span, :]
        scores = dot_last(kbuf[z, part, :], qq) * scale + (stat_row(1, a, c) - wide(0, part))
        if masked:
            s = lax.broadcasted_iota(jnp.int32, scores.shape, 0) + part.start
            t = lax.broadcasted_iota(jnp.int32, scores.shape, 1) + c * width
            scores = jnp.where(s <= t, scores, -jnp.inf)
        weights = jnp.exp(scores)
        slopes = weights * (dot_last(vbuf[z, part, :], dd) - stat_row(2, a, c))
        acc[1, part, :] += dot_plain(slopes.astype(BF16), qq)
        acc[2, part, :] += dot_plain(weights.astype(BF16), dd)

    acc[...] = jnp.zeros_like(acc)
    chunks = length // width
    for c in range(chunks):
        query_tile(z, c, slice(c * width, length), True)

    @pl.loop(1, z + 1)
    def _(k):
        for j in range(u):
            wait_stat(k, j)
            wait_main(0, k, j)
            wait_main(1, k, j)
        for c in range(chunks):
            query_tile(z - k, c, slice(0, length), False)

    dqpair[p] = (acc[0] * scale).astype(BF16)
    for j in range(u):
        here = xbuf.at[rows(source_of(j)), :]
        pltpu.make_async_copy(here, here, x_recv.at[j]).wait()

    def pair_copy(j):
        return remote(
            dqpair.at[p], dqpair.at[p], pair_send.at[j], pair_recv.at[j], me, lax.rem(p + j, tp)
        )

    for j in range(1, tp):
        pair_copy(j).start()

    outs = (dq_out, dk_out, dv_out)

    def out_source(m, h):
        return dqpair.at[p, rows(h), :] if m == 0 else dkv.at[m - 1, rows(h), :]

    def out_copy(m, j):
        h = head_of(j)
        return remote(
            out_source(m, h), outs[m].at[:, lanes(g)],
            out_send.at[m, j], out_recv.at[m, j], z * u + h, p,
        )

    def out_own(m):
        return pltpu.make_async_copy(
            out_source(m, g), outs[m].at[:, lanes(g)], out_recv.at[m, 0]
        )

    for c in range(chunks):
        key_tile(z, c, slice(0, (c + 1) * width), True)

    for j in range(1, tp):
        there = dqpair.at[lax.rem(p + tp - j, tp)]
        pltpu.make_async_copy(there, there, pair_recv.at[j]).wait()
    both = jnp.concatenate([dqpair[t] for t in range(tp)], axis=1)

    def w_copy(o, t):
        return remote(
            wsend.at[o, t], wrecv.at[me], w_send.at[o, t], w_recv.at[me], p * owners + o, t
        )

    def w_send_out(o):
        for t in range(tp):
            mine = jnp.logical_and(p * owners + o == me, p == t)

            @pl.when(mine)
            def _():
                pltpu.make_async_copy(wsend.at[o, t], wrecv.at[me], w_recv.at[me]).start()

            @pl.when(jnp.logical_not(mine))
            def _():
                w_copy(o, t).start()

    for o in range(owners):
        block = dot_first(xbuf[:, o * fw : (o + 1) * fw], both).astype(BF16)
        for t in range(tp):
            wsend[o, t] = block[:, t * hd : (t + 1) * hd]
        if o:
            w_send_out(o - 1)
    for j in range(1, u):
        out_copy(0, j).start()
    out_own(0).start()
    w_send_out(owners - 1)

    @pl.loop(1, r - z)
    def _(k):
        for j in range(u):
            wait_stat(-k, j)
            wait_main(2, k, j)
            wait_main(3, k, j)
        for c in range(chunks):
            key_tile(z + k, c, slice(0, length), False)

    dkv[0] = (acc[1] * scale).astype(BF16)
    dkv[1] = acc[2].astype(BF16)

    for i in range(sp):
        pltpu.make_async_copy(wrecv.at[i], wrecv.at[i], w_recv.at[i]).wait()
    for m in (1, 2):
        for j in range(1, u):
            out_copy(m, j).start()
        out_own(m).start()
    for h in range(u):
        total = wrecv[h].astype(F32)
        for layer in range(1, r):
            total += wrecv[layer * u + h].astype(F32)
        w_out[:, h * hd : (h + 1) * hd] = total

    each_send(lambda copy: copy.wait_send())
    for j in range(1, tp):
        pair_copy(j).wait_send()
    for o in range(owners):
        for t in range(tp):

            @pl.when(jnp.logical_not(jnp.logical_and(p * owners + o == me, p == t)))
            def _():
                w_copy(o, t).wait_send()

    for m in range(3):
        for j in range(u):
            here = outs[m].at[:, lanes(source_of(j))]
            pltpu.make_async_copy(here, here, out_recv.at[m, j]).wait()
            if j:
                out_copy(m, j).wait_send()


def fused_device(sp, tp, *arrays):
    n, row_width = arrays[0].shape
    u = arrays[3].shape[1]
    hd = row_width // u
    r = sp // u
    length = u * n
    features = arrays[7].shape[1]
    owners = sp // tp
    fw = features // owners
    vmem = pl.BlockSpec(memory_space=pltpu.VMEM)
    dma = pltpu.SemaphoreType.DMA
    narrow = jax.ShapeDtypeStruct((n, row_width), BF16)
    return pl.pallas_call(
        functools.partial(fused_kernel, sp, tp, u, n, hd),
        out_shape=(narrow, narrow, narrow, jax.ShapeDtypeStruct((fw, row_width), F32)),
        in_specs=[vmem] * 8,
        out_specs=(vmem,) * 4,
        scratch_shapes=[
            pltpu.VMEM((r, length, hd), BF16),
            pltpu.VMEM((r, length, hd), BF16),
            pltpu.VMEM((r, length, hd), BF16),
            pltpu.VMEM((r, length, hd), BF16),
            pltpu.VMEM((sp, 8, n), F32),
            pltpu.VMEM((u, 8, n), F32),
            pltpu.VMEM((2, n, hd), F32),
            pltpu.VMEM((3, length, hd), F32),
            pltpu.VMEM((length, features), BF16),
            pltpu.VMEM((tp, length, hd), BF16),
            pltpu.VMEM((2, length, hd), BF16),
            pltpu.VMEM((3, length, hd), F32),
            pltpu.VMEM((owners, tp, fw, hd), BF16),
            pltpu.VMEM((sp, fw, hd), BF16),
            dma((4, r, u)), dma((4, r, u)),
            dma((2 * r - 1, u)), dma((2 * r - 1, u)),
            dma((u,)), dma((u,)),
            dma((tp,)), dma((tp,)),
            dma((3, u)), dma((3, u)),
            dma((owners, tp)), dma((sp,)),
        ],
        compiler_params=pltpu.CompilerParams(
            collective_id=0, has_side_effects=True, vmem_limit_bytes=48 * 1024 * 1024
        ),
    )(*arrays)


def fits(sp, tp, heads, n, hd):
    return heads > 1 and sp % heads == 0 and sp % tp == 0 and n == hd


def solution(mesh):
    sp, tp = mesh.shape["sp"], mesh.shape["tp"]

    def per_device(*arrays):
        heads = arrays[3].shape[1]
        n, row_width = arrays[0].shape
        if fits(sp, tp, heads, n, row_width // heads):
            return fused_device(sp, tp, *arrays)
        return gathered_device(*arrays)

    return jax.shard_map(
        per_device,
        mesh=mesh,
        in_specs=(
            P("sp", "tp"),
            P("sp", "tp"),
            P("sp", "tp"),
            P("sp", "tp"),
            P("sp", "tp"),
            P("sp", "tp"),
            P("sp", "tp"),
            P("sp", "tp"),
        ),
        out_specs=(P("sp", "tp"), P("sp", "tp"), P("sp", "tp"), P("sp", "tp")),
        check_vma=False,
    )
```

```python
import functools

import jax
import jax.numpy as jnp
from jax import lax
from jax.experimental import pallas as pl
from jax.experimental.pallas import tpu as pltpu
from jax.sharding import PartitionSpec as P


def block_length(whole_rows):
    length = whole_rows
    while length > 1024 and length % 2 == 0:
        length = length // 2
    return length


def split_heads(block, head_count):
    return block.reshape(block.shape[0], head_count, block.shape[1] // head_count)


def attention_weights(
    query_part, key_part, norm_part, gate_query, gate_key, query_pos, key_pos, score_scale
):
    scores = (
        jnp.einsum("ahd,bhd->hab", query_part, key_part, preferred_element_type=jnp.float32)
        * score_scale
    )
    scores = scores + (gate_query.T[:, :, None] - gate_key.T[:, None, :])
    allowed = key_pos[None, None, :] <= query_pos[None, :, None]
    return jnp.exp(jnp.where(allowed, scores - norm_part.T[:, :, None], -jnp.inf))


def score_slopes(weights, grad_part, value_part, term_part):
    flows = jnp.einsum("ahd,bhd->hab", grad_part, value_part, preferred_element_type=jnp.float32)
    return weights * (flows - term_part.T[:, :, None])


def over_blocks(visit_block, running, members):
    whole_rows = members[0].shape[0]
    length = block_length(whole_rows)
    number = whole_rows // length
    stacked = tuple((member.reshape((number, length) + member.shape[1:]) for member in members))

    def visit_one(carried, scanned):
        block_index, block_parts = scanned
        token_places = block_index * length + jnp.arange(length, dtype=jnp.int32)
        return (visit_block(carried, block_parts, token_places), None)

    result, unused = lax.scan(visit_one, running, (jnp.arange(number, dtype=jnp.int32), stacked))
    return result


def gathered_device(
    query_heads,
    key_heads,
    value_heads,
    decay_sums,
    row_logsums,
    head_outputs,
    out_cotangent,
    normed_input,
):
    own_rows, row_width = query_heads.shape
    head_count = decay_sums.shape[1]
    score_scale = (row_width // head_count) ** (-0.5)
    own_pos = lax.axis_index("sp") * own_rows + jnp.arange(own_rows, dtype=jnp.int32)
    own_query = split_heads(query_heads, head_count)
    own_key = split_heads(key_heads, head_count)
    own_value = split_heads(value_heads, head_count)
    own_grad = split_heads(out_cotangent, head_count)
    row_terms = jnp.einsum(
        "ahd,ahd->ah",
        split_heads(head_outputs, head_count),
        own_grad,
        preferred_element_type=jnp.float32,
    )
    all_gates, all_logsums, all_terms = (
        lax.all_gather(decay_sums, "sp", axis=0, tiled=True),
        lax.all_gather(row_logsums, "sp", axis=0, tiled=True),
        lax.all_gather(row_terms, "sp", axis=0, tiled=True),
    )

    def query_side(query_sum, key_part, value_part, key_pos):
        gate_key = lax.dynamic_slice_in_dim(all_gates, key_pos[0], key_pos.shape[0], 0)

        def query_compute(running):
            weights = attention_weights(
                own_query,
                key_part,
                row_logsums,
                decay_sums,
                gate_key,
                own_pos,
                key_pos,
                score_scale,
            )
            slopes = score_slopes(weights, own_grad, value_part, row_terms)
            return running + jnp.einsum(
                "hab,bhd->ahd",
                slopes.astype(jnp.bfloat16),
                key_part,
                preferred_element_type=jnp.float32,
            )

        return lax.cond(
            key_pos[0] <= own_pos[-1], query_compute, lambda running: running, query_sum
        )

    def key_side(key_sums, query_part, grad_part, query_pos):
        length = query_pos.shape[0]
        gate_query = lax.dynamic_slice_in_dim(all_gates, query_pos[0], length, 0)
        norm_part = lax.dynamic_slice_in_dim(all_logsums, query_pos[0], length, 0)
        term_part = lax.dynamic_slice_in_dim(all_terms, query_pos[0], length, 0)

        def key_compute(running):
            key_sum, value_sum = running
            weights = attention_weights(
                query_part,
                own_key,
                norm_part,
                gate_query,
                decay_sums,
                query_pos,
                own_pos,
                score_scale,
            )
            slopes = score_slopes(weights, grad_part, own_value, term_part)
            key_sum = key_sum + jnp.einsum(
                "hab,ahd->bhd",
                slopes.astype(jnp.bfloat16),
                query_part,
                preferred_element_type=jnp.float32,
            )
            value_sum = value_sum + jnp.einsum(
                "hab,ahd->bhd",
                weights.astype(jnp.bfloat16),
                grad_part,
                preferred_element_type=jnp.float32,
            )
            return (key_sum, value_sum)

        return lax.cond(query_pos[-1] >= own_pos[0], key_compute, lambda running: running, key_sums)

    zero_sums = jnp.zeros((own_rows, head_count, row_width // head_count), jnp.float32)

    def visit_block(carried, block_parts, token_places):
        return query_side(
            carried,
            split_heads(block_parts[0], head_count),
            split_heads(block_parts[1], head_count),
            token_places,
        )

    query_sum = over_blocks(
        visit_block,
        zero_sums,
        (
            lax.all_gather(key_heads, "sp", axis=0, tiled=True),
            lax.all_gather(value_heads, "sp", axis=0, tiled=True),
        ),
    )

    def visit_block(carried, block_parts, token_places):
        return key_side(
            carried,
            split_heads(block_parts[0], head_count),
            split_heads(block_parts[1], head_count),
            token_places,
        )

    key_sum, value_sum = over_blocks(
        visit_block,
        (zero_sums, zero_sums),
        (
            lax.all_gather(query_heads, "sp", axis=0, tiled=True),
            lax.all_gather(out_cotangent, "sp", axis=0, tiled=True),
        ),
    )
    query_grads = (query_sum * score_scale).astype(jnp.bfloat16).reshape(own_rows, row_width)
    key_grads = (key_sum * score_scale).astype(jnp.bfloat16).reshape(own_rows, row_width)
    value_grads = value_sum.astype(jnp.bfloat16).reshape(own_rows, row_width)
    whole_input = lax.all_gather(normed_input, "tp", axis=1, tiled=True)
    own_features = lax.all_to_all(whole_input, "sp", split_axis=1, concat_axis=0, tiled=True)
    weight_grad = lax.dot_general(
        own_features,
        lax.all_gather(query_grads, "sp", axis=0, tiled=True),
        (((0,), (0,)), ((), ())),
        preferred_element_type=jnp.float32,
    )
    return (query_grads, key_grads, value_grads, weight_grad)


F32 = jnp.float32
BF16 = jnp.bfloat16


def dot_last(a, b):
    return lax.dot_general(a, b, (((1,), (1,)), ((), ())), preferred_element_type=F32)


def dot_plain(a, b):
    return lax.dot_general(a, b, (((1,), (0,)), ((), ())), preferred_element_type=F32)


def dot_first(a, b):
    return lax.dot_general(a, b, (((0,), (0,)), ((), ())), preferred_element_type=F32)


def fused_kernel(
    sp, tp, u, n, hd,
    q_hbm, k_hbm, v_hbm, g_ref, l_ref, o_hbm, do_hbm, x_ref,
    dq_out, dk_out, dv_out, wrecv,
    held, kbuf, vbuf, qbuf, dobuf, sbuf, ssend, cols, xbuf, dqpair, dkv, acc, wsend,
    main_send, main_recv, stat_send, stat_recv, x_send, x_recv,
    pair_send, pair_recv, out_send, out_recv, w_send, w_recv, load_sem, relay_send,
):
    r = sp // u
    length = u * n
    owners = sp // tp
    fw = x_ref.shape[1] // owners
    scale = hd ** (-0.5)
    me, p = lax.axis_index("sp"), lax.axis_index("tp")
    z, g = me // u, me % u

    def lanes(index, width=hd):
        return pl.ds(pl.multiple_of(index * width, width), width)

    def rows(index):
        return pl.ds(pl.multiple_of(index * n, n), n)

    def remote(src, dst, send, recv, i, t):
        return pltpu.make_async_remote_copy(
            src_ref=src, dst_ref=dst, send_sem=send, recv_sem=recv,
            device_id={"sp": i, "tp": t}, device_id_type=pl.DeviceIdType.MESH,
        )

    operands = (o_hbm, do_hbm, q_hbm, k_hbm, v_hbm)
    loads = [pltpu.make_async_copy(ref, held.at[i], load_sem.at[i]) for i, ref in enumerate(operands)]
    for load in loads:
        load.start()
    o_ref, do_ref, q_ref, k_ref, v_ref = (held.at[i] for i in range(5))
    barrier = pltpu.get_barrier_semaphore()
    for d in range(1, sp * tp):
        other = lax.rem(me * tp + p + d, sp * tp)
        pl.semaphore_signal(
            barrier, inc=1, device_id={"sp": other // tp, "tp": other % tp},
            device_id_type=pl.DeviceIdType.MESH,
        )

    loads[0].wait()
    loads[1].wait()
    lane = lax.broadcasted_iota(jnp.int32, (n, hd), 1)
    terms = jnp.zeros((n, hd), F32)
    for h in range(u):
        part = slice(h * hd, (h + 1) * hd)
        total = jnp.sum(
            o_ref[:, part].astype(F32) * do_ref[:, part].astype(F32), axis=1, keepdims=True
        )
        terms = jnp.where(lane == h, total, terms)
    flat = (g_ref[...], g_ref[...] - l_ref[...], terms.T)
    for h in range(u):
        for s in range(3):
            ssend[h, s : s + 1, :] = flat[s][h : h + 1, :]
    for load in loads[2:]:
        load.wait()
    pl.semaphore_wait(barrier, sp * tp - 1)

    def head_of(j):
        return lax.rem(g + j, u)

    def source_of(j):
        return lax.rem(g + u - j, u)

    pairs = ((k_ref, kbuf), (v_ref, vbuf), (q_ref, qbuf), (do_ref, dobuf))

    def main_copy(a, k, j):
        ref, buf = pairs[a]
        layer = z + k if a < 2 else z - k
        h = head_of(j)
        return remote(
            ref.at[:, lanes(h)], buf.at[z, rows(g), :],
            main_send.at[a, k, j], main_recv.at[a, k, j], layer * u + h, p,
        )

    def own_copy(a):
        ref, buf = pairs[a]
        return pltpu.make_async_copy(
            ref.at[:, lanes(g)], buf.at[z, rows(g), :], main_recv.at[a, 0, 0]
        )

    def wait_main(a, k, j):
        ref, buf = pairs[a]
        layer = z - k if a < 2 else z + k
        here = buf.at[layer, rows(source_of(j)), :]
        pltpu.make_async_copy(here, here, main_recv.at[a, k, j]).wait()

    def stat_copy(d, j):
        h = head_of(j)
        return remote(
            ssend.at[h], sbuf.at[me], stat_send.at[d + r - 1, j], stat_recv.at[d + r - 1, j],
            (z + d) * u + h, p,
        )

    def wait_stat(d, j):
        here = sbuf.at[(z - d) * u + source_of(j)]
        pltpu.make_async_copy(here, here, stat_recv.at[d + r - 1, j]).wait()

    def own_stat():
        return pltpu.make_async_copy(ssend.at[g], sbuf.at[me], stat_recv.at[r - 1, 0])

    def x_copy(j):
        return remote(
            x_ref, xbuf.at[rows(g), :], x_send.at[j], x_recv.at[j], z * u + head_of(j), p
        )

    def up(k):
        return z + k < r

    def down(k):
        return z >= k

    def relay(a, k):
        buf = pairs[a][1]
        layer, step = (z - k, 1) if a < 2 else (z + k, -1)
        return remote(
            buf.at[layer], buf.at[layer], relay_send.at[a, k], main_recv.at[a, k + 1, 0],
            (z + step) * u + g, p,
        )

    def wait_layer(a, k):
        if k < 3:
            for j in range(u):
                wait_main(a, k, j)
        else:
            here = pairs[a][1].at[z - k if a < 2 else z + k]
            pltpu.make_async_copy(here, here, main_recv.at[a, k, 0]).wait()

    order = [k for k in (2, 1) if k < r] + list(range(3, r))

    def each_send(act):
        for j in range(1, u):
            act(stat_copy(0, j))
        for a in (2, 0, 3, 1):
            for j in range(1, u):
                act(main_copy(a, 0, j))
        for k in order:
            for reach, sign, members in ((up, 1, (0, 1)), (down, -1, (2, 3))):

                @pl.when(reach(k))
                def _(k=k, sign=sign, members=members):
                    for j in range(u):
                        act(stat_copy(sign * k, j))
                    for a in members:
                        for j in range(u):
                            if k < 3:
                                act(main_copy(a, k, j))

        for j in range(1, u):
            act(x_copy(j))

    each_send(lambda copy: copy.start())
    own_stat().start()
    for a in range(4):
        own_copy(a).start()
    own_x = pltpu.make_async_copy(x_ref, xbuf.at[rows(g), :], x_recv.at[0])
    own_x.start()

    for j in range(u):
        wait_stat(0, j)
        for a in range(4):
            wait_main(a, 0, j)
    for b in range(u):
        for s in range(3):
            row = sbuf[z * u + b, s : s + 1, :]
            cols[s, b * n : (b + 1) * n, :] = jnp.broadcast_to(row, (hd, n)).T

    width = 2 * n if u % 2 == 0 else n
    pieces = width // n

    def stat_row(s, layer, c):
        return jnp.concatenate(
            [sbuf[layer * u + c * pieces + i, s : s + 1, :] for i in range(pieces)], axis=1
        )

    def wide(s, part):
        return jnp.concatenate([cols[s, part, :]] * pieces, axis=1)

    def query_tile(b, c, part, masked):
        keys = slice(c * width, (c + 1) * width)
        kk, vv = kbuf[b, keys, :], vbuf[b, keys, :]
        scores = dot_last(qbuf[z, part, :], kk) * scale + (wide(1, part) - stat_row(0, b, c))
        if masked:
            t = lax.broadcasted_iota(jnp.int32, scores.shape, 0) + part.start
            s = lax.broadcasted_iota(jnp.int32, scores.shape, 1) + c * width
            scores = jnp.where(s <= t, scores, -jnp.inf)
        slopes = jnp.exp(scores) * (dot_last(dobuf[z, part, :], vv) - wide(2, part))
        acc[0, part, :] += dot_plain(slopes.astype(BF16), kk)

    def key_tile(a, c, part, masked):
        span = slice(c * width, (c + 1) * width)
        qq, dd = qbuf[a, span, :], dobuf[a, span, :]
        scores = dot_last(kbuf[z, part, :], qq) * scale + (stat_row(1, a, c) - wide(0, part))
        if masked:
            s = lax.broadcasted_iota(jnp.int32, scores.shape, 0) + part.start
            t = lax.broadcasted_iota(jnp.int32, scores.shape, 1) + c * width
            scores = jnp.where(s <= t, scores, -jnp.inf)
        weights = jnp.exp(scores)
        slopes = weights * (dot_last(vbuf[z, part, :], dd) - stat_row(2, a, c))
        acc[1, part, :] += dot_plain(slopes.astype(BF16), qq)
        acc[2, part, :] += dot_plain(weights.astype(BF16), dd)

    acc[...] = jnp.zeros_like(acc)
    chunks = length // width
    for c in range(chunks):
        query_tile(z, c, slice(c * width, length), True)

    def passes(k):
        far = 2 <= k < r - 1
        return (jnp.logical_and(down(k), z + 1 < r) if far else None,
                jnp.logical_and(up(k), z >= 1) if far else None)

    for k in order:
        onward, back = passes(k)
        if back is not None:

            @pl.when(back)
            def _():
                wait_layer(2, k)
                relay(2, k).start()
                wait_layer(3, k)
                relay(3, k).start()

        if onward is not None:

            @pl.when(onward)
            def _():
                wait_layer(0, k)
                relay(0, k).start()
                wait_layer(1, k)
                relay(1, k).start()

        @pl.when(down(k))
        def _():
            for j in range(u):
                wait_stat(k, j)
            if onward is None:
                wait_layer(0, k)
                wait_layer(1, k)
            else:

                @pl.when(jnp.logical_not(onward))
                def _():
                    wait_layer(0, k)
                    wait_layer(1, k)

            for c in range(chunks):
                query_tile(z - k, c, slice(0, length), False)

    dqpair[p] = (acc[0] * scale).astype(BF16)
    for j in range(u):
        here = xbuf.at[rows(source_of(j)), :]
        pltpu.make_async_copy(here, here, x_recv.at[j]).wait()

    def pair_copy(j):
        return remote(
            dqpair.at[p], dqpair.at[p], pair_send.at[j], pair_recv.at[j], me, lax.rem(p + j, tp)
        )

    for j in range(1, tp):
        pair_copy(j).start()

    outs = (dq_out, dk_out, dv_out)

    def out_source(m, h):
        return dqpair.at[p, rows(h), :] if m == 0 else dkv.at[m - 1, rows(h), :]

    def out_copy(m, j):
        h = head_of(j)
        return remote(
            out_source(m, h), outs[m].at[:, lanes(g)],
            out_send.at[m, j], out_recv.at[m, j], z * u + h, p,
        )

    def out_own(m):
        return pltpu.make_async_copy(
            out_source(m, g), outs[m].at[:, lanes(g)], out_recv.at[m, 0]
        )

    for c in range(chunks):
        key_tile(z, c, slice(0, (c + 1) * width), True)

    for j in range(1, tp):
        there = dqpair.at[lax.rem(p + tp - j, tp)]
        pltpu.make_async_copy(there, there, pair_recv.at[j]).wait()
    both = jnp.concatenate([dqpair[t] for t in range(tp)], axis=1)

    def w_copy(o, t):
        return remote(
            wsend.at[o, t], wrecv.at[me], w_send.at[o, t], w_recv.at[me], p * owners + o, t
        )

    def w_send_out(o):
        for t in range(tp):
            mine = jnp.logical_and(p * owners + o == me, p == t)

            @pl.when(mine)
            def _():
                pltpu.make_async_copy(wsend.at[o, t], wrecv.at[me], w_recv.at[me]).start()

            @pl.when(jnp.logical_not(mine))
            def _():
                w_copy(o, t).start()

    for o in range(owners):
        block = dot_first(xbuf[:, o * fw : (o + 1) * fw], both).astype(BF16)
        for t in range(tp):
            wsend[o, t] = block[:, t * hd : (t + 1) * hd]
        if o:
            w_send_out(o - 1)
    for j in range(1, u):
        out_copy(0, j).start()
    out_own(0).start()
    w_send_out(owners - 1)

    for k in order:
        back = passes(k)[1]

        @pl.when(up(k))
        def _():
            for j in range(u):
                wait_stat(-k, j)
            if back is None:
                wait_layer(2, k)
                wait_layer(3, k)
            else:

                @pl.when(jnp.logical_not(back))
                def _():
                    wait_layer(2, k)
                    wait_layer(3, k)

            for c in range(chunks):
                key_tile(z + k, c, slice(0, length), False)

    dkv[0] = (acc[1] * scale).astype(BF16)
    dkv[1] = acc[2].astype(BF16)

    each_send(lambda copy: copy.wait_send())
    for j in range(1, tp):
        pair_copy(j).wait_send()
    for k in order:
        onward, back = passes(k)
        for gate, members in ((onward, (0, 1)), (back, (2, 3))):
            if gate is not None:

                @pl.when(gate)
                def _():
                    for a in members:
                        relay(a, k).wait_send()

    for m in (1, 2):
        for j in range(1, u):
            out_copy(m, j).start()
        out_own(m).start()
    for i in range(sp):
        pltpu.make_async_copy(wrecv.at[i], wrecv.at[i], w_recv.at[i]).wait()
    for o in range(owners):
        for t in range(tp):

            @pl.when(jnp.logical_not(jnp.logical_and(p * owners + o == me, p == t)))
            def _():
                w_copy(o, t).wait_send()

    for m in range(3):
        for j in range(u):
            here = outs[m].at[:, lanes(source_of(j))]
            pltpu.make_async_copy(here, here, out_recv.at[m, j]).wait()
            if j:
                out_copy(m, j).wait_send()


def finish_kernel(sp, u, hd, dq, dk, dv, parts, dq_out, dk_out, dv_out, w_out, total, sems):
    copies = [
        pltpu.make_async_copy(src, dst, sems.at[i])
        for i, (src, dst) in enumerate(
            ((dq, dq_out), (dk, dk_out), (dv, dv_out), (total, w_out))
        )
    ]
    for copy in copies[:3]:
        copy.start()
    for h in range(u):
        running = parts[h].astype(F32)
        for i in range(h + u, sp, u):
            running += parts[i].astype(F32)
        total[:, h * hd : (h + 1) * hd] = running
    copies[3].start()
    for copy in copies:
        copy.wait()


def fused_device(sp, tp, *arrays):
    n, row_width = arrays[0].shape
    u = arrays[3].shape[1]
    hd = row_width // u
    r = sp // u
    length = u * n
    features = arrays[7].shape[1]
    owners = sp // tp
    fw = features // owners
    vmem = pl.BlockSpec(memory_space=pltpu.VMEM)
    hbm = pl.BlockSpec(memory_space=pl.ANY)
    dma = pltpu.SemaphoreType.DMA
    narrow = jax.ShapeDtypeStruct((n, row_width), BF16)
    parts = pl.pallas_call(
        functools.partial(fused_kernel, sp, tp, u, n, hd),
        out_shape=(narrow, narrow, narrow, jax.ShapeDtypeStruct((sp, fw, hd), BF16)),
        in_specs=[hbm, hbm, hbm, vmem, vmem, hbm, hbm, hbm],
        out_specs=(vmem,) * 4,
        scratch_shapes=[
            pltpu.VMEM((5, n, row_width), BF16),
            pltpu.VMEM((r, length, hd), BF16),
            pltpu.VMEM((r, length, hd), BF16),
            pltpu.VMEM((r, length, hd), BF16),
            pltpu.VMEM((r, length, hd), BF16),
            pltpu.VMEM((sp, 8, n), F32),
            pltpu.VMEM((u, 8, n), F32),
            pltpu.VMEM((3, length, hd), F32),
            pltpu.VMEM((length, features), BF16),
            pltpu.VMEM((tp, length, hd), BF16),
            pltpu.VMEM((2, length, hd), BF16),
            pltpu.VMEM((3, length, hd), F32),
            pltpu.VMEM((owners, tp, fw, hd), BF16),
            dma((4, r, u)), dma((4, r, u)),
            dma((2 * r - 1, u)), dma((2 * r - 1, u)),
            dma((u,)), dma((u,)),
            dma((tp,)), dma((tp,)),
            dma((3, u)), dma((3, u)),
            dma((owners, tp)), dma((sp,)), dma((5,)), dma((4, r)),
        ],
        compiler_params=pltpu.CompilerParams(
            collective_id=0, has_side_effects=True
        ),
    )(*arrays[:3], arrays[3].T, arrays[4].T, *arrays[5:])
    return pl.pallas_call(
        functools.partial(finish_kernel, sp, u, hd),
        out_shape=(narrow, narrow, narrow, jax.ShapeDtypeStruct((fw, row_width), F32)),
        in_specs=[vmem] * 4,
        out_specs=(hbm,) * 4,
        scratch_shapes=[pltpu.VMEM((fw, row_width), F32), dma((4,))],
    )(*parts)


def fits(sp, tp, heads, n, hd):
    return heads > 1 and sp % heads == 0 and sp % tp == 0 and n == hd


def solution(mesh):
    sp, tp = mesh.shape["sp"], mesh.shape["tp"]

    def per_device(*arrays):
        heads = arrays[3].shape[1]
        n, row_width = arrays[0].shape
        if fits(sp, tp, heads, n, row_width // heads):
            return fused_device(sp, tp, *arrays)
        return gathered_device(*arrays)

    return jax.shard_map(
        per_device,
        mesh=mesh,
        in_specs=(
            P("sp", "tp"),
            P("sp", "tp"),
            P("sp", "tp"),
            P("sp", "tp"),
            P("sp", "tp"),
            P("sp", "tp"),
            P("sp", "tp"),
            P("sp", "tp"),
        ),
        out_specs=(P("sp", "tp"), P("sp", "tp"), P("sp", "tp"), P("sp", "tp")),
        check_vma=False,
    )
```
